32 devices in a mesh: sp: 8 (over z, y), tp: 4 (over x, core).
Axes of the slice: x: 2, y: 2, z: 4, core: 2. Of those that a mesh axis runs over, the one named last changes fastest.
Arguments:
- resid: bfloat16 [4096, 2048], P('sp', 'tp'), may hold values from -41 to 41
- queries: bfloat16 [4096, 1024], P('sp', 'tp'), may hold values from -6 to 6
- keys: bfloat16 [4096, 1024], P('sp', 'tp'), may hold values from -6 to 6
- values: bfloat16 [4096, 1024], P('sp', 'tp'), may hold values from -6 to 6
- mix_lambda: float32 [8], P('tp'), may hold values from 0.3 to 0.8
- head_gain: float32 [128], replicated, may hold values from 0.1 to 1.9
- out_weight: bfloat16 [1024, 2048], P(None, 'tp'), may hold values from -0.1875 to 0.1875
- norm_gain: float32 [2048], P('tp'), may hold values from 0.1 to 1.9
- gate_weight: bfloat16 [2048, 5632], P('sp', 'tp'), may hold values from -0.125 to 0.125
- up_weight: bfloat16 [2048, 5632], P('sp', 'tp'), may hold values from -0.125 to 0.125
- conv_weight: float32 [3, 5632], P(None, 'tp'), may hold values from -3.5 to 3.5
- conv_bias: float32 [5632], P('tp'), may hold values from -3 to 3
- down_weight: bfloat16 [5632, 2048], P('tp', 'sp'), may hold values from -0.078125 to 0.078125
Outputs:
- layer_out: bfloat16 [4096, 2048], P('sp', 'tp')
The draws below stay inside these ranges and needn't reach their ends.
All inputs are finite; a program needn't handle non-finite values.
Results may differ from the reference program's by a relative error of at most 0.009.
Values may be sent and summed in bfloat16 or wider, within the bound.
A program may use at most 128 MiB of HBM per device.

```python
import math
import jax
import jax.numpy as jnp
from jax import lax

D = 2048
HEADS = 8
HD = 64
VD = 128
FF = 5632
TOKENS = 4096
N_TP = 4


def pair_draw(key):
    width = HEADS * 2 * HD
    query_part = 1.3 * jnp.clip(jax.random.normal(jax.random.fold_in(key, 11), (TOKENS, width), jnp.float32), -4.0, 4.0)
    key_part = 1.3 * jnp.clip(jax.random.normal(jax.random.fold_in(key, 12), (TOKENS, width), jnp.float32), -4.0, 4.0)
    return (query_part, key_part)


def draw_queries(key, part):
    return pair_draw(key)[0].astype(jnp.bfloat16)


def draw_keys(key, part):
    return pair_draw(key)[1].astype(jnp.bfloat16)


def draw_resid(key, part):
    base = jax.random.fold_in(key, 21)
    row_scale = 10.0 ** (jax.random.uniform(jax.random.fold_in(base, 1), (TOKENS, 1), jnp.float32) - 0.5)
    position = jnp.arange(D, dtype=jnp.float32)[None, :] / D
    column_scale = 10.0 ** (0.7 * position + 0.3 * jax.random.uniform(jax.random.fold_in(base, 2), (1, D), jnp.float32) - 0.5)
    noise = jnp.clip(jax.random.normal(jax.random.fold_in(base, 4), (TOKENS, D), jnp.float32), -4.0, 4.0)
    return (noise * row_scale * column_scale).astype(jnp.bfloat16)


def levels(own_key, extent, pieces, smallest, high):
    loudness = 1.0
    for dim, blocks in pieces:
        steps = jax.random.uniform(jax.random.fold_in(jax.random.fold_in(own_key, 6), dim), (blocks,), jnp.float32, smallest / len(pieces), high / len(pieces))
        loudness = loudness * jnp.repeat(jnp.exp(steps), extent[dim] // blocks).reshape((-1,) + (1,) * (len(extent) - 1 - dim))
    return loudness


def normal_values(own_key, extent, scale, most, cuts=(), kind=jnp.bfloat16):
    level = levels(own_key, extent, cuts, -0.22, 0.18) if cuts else 1.0
    result = jax.random.normal(own_key, extent, jnp.float32) * scale * level
    return jnp.minimum(jnp.maximum(result, -most), most).astype(kind)


def setup_inputs(seed: int = 0) -> dict:
    arg_keys = jax.random.split(jax.random.key(seed), 14)
    resid = draw_resid(jax.random.fold_in(arg_keys[13], 71), 0)
    queries = draw_queries(jax.random.fold_in(arg_keys[13], 71), 0)
    keys = draw_keys(jax.random.fold_in(arg_keys[13], 71), 0)
    values = normal_values(arg_keys[3], (TOKENS, HEADS * VD), 1.0, 6.0, ((0, 8), (1, 4)))
    mix_lambda = jnp.clip(0.3 + 0.5 * jax.random.uniform(arg_keys[4], (HEADS,), jnp.float32) ** levels(arg_keys[4], (HEADS,), ((0, 4),), -0.2, 0.2), 0.3, 0.8)
    head_gain = jnp.clip(1.0 + 0.18 * jax.random.normal(arg_keys[5], (VD,), jnp.float32), 0.1, 1.9)
    out_weight = normal_values(arg_keys[6], (HEADS * VD, D), (HEADS * VD) ** -0.5, 0.1875, ((1, 4),))
    norm_gain = jnp.clip(1.0 + 0.18 * jax.random.normal(arg_keys[7], (D,), jnp.float32), 0.1, 1.9)
    gate_weight = normal_values(arg_keys[8], (D, FF), D ** -0.5, 0.125, ((0, 8), (1, 4)))
    up_weight = normal_values(arg_keys[9], (D, FF), D ** -0.5, 0.125, ((0, 8), (1, 4)))
    conv_weight = normal_values(arg_keys[10], (3, FF), 3 ** -0.5, 3.5, ((1, 4),), jnp.float32)
    conv_bias = normal_values(arg_keys[11], (FF,), 0.5, 3.0, ((0, 4),), jnp.float32)
    down_weight = normal_values(arg_keys[12], (FF, D), FF ** -0.5, 0.078125, ((0, 4), (1, 8)))
    return {"resid": resid, "queries": queries, "keys": keys, "values": values, "mix_lambda": mix_lambda, "head_gain": head_gain, "out_weight": out_weight, "norm_gain": norm_gain, "gate_weight": gate_weight, "up_weight": up_weight, "conv_weight": conv_weight, "conv_bias": conv_bias, "down_weight": down_weight}


def head_attention(query_head, key_head, value_head, weight_two):
    length = query_head.shape[0]
    scale = HD ** (-0.5)
    block = math.gcd(length, 512)
    query_blocks = query_head.reshape(length // block, block, 2, HD)
    key_float = key_head.astype(jnp.float32)
    value_float = value_head.astype(jnp.float32)

    def one_block(query_block):
        scores = jnp.einsum('qmd,kmd->mqk', query_block.astype(jnp.float32), key_float) * scale
        highest = lax.optimization_barrier(jnp.max(scores, axis=-1, keepdims=True))
        shifted = jnp.exp(scores - highest)
        totals = lax.optimization_barrier(jnp.sum(shifted, axis=-1))
        unnormed = lax.optimization_barrier(shifted.astype(jnp.bfloat16)).astype(jnp.float32)
        mapped = jnp.einsum('mqk,ke->mqe', unnormed, value_float) / totals[..., None]
        return mapped[0] - weight_two * mapped[1]
    return lax.map(one_block, query_blocks).reshape(length, VD)

def reference(resid, queries, keys, values, mix_lambda, head_gain, out_weight, norm_gain, gate_weight, up_weight, conv_weight, conv_bias, down_weight):
    length = queries.shape[0]
    query_heads = jnp.transpose(queries.reshape(length, HEADS, 2, HD), (1, 0, 2, 3))
    key_heads = jnp.transpose(keys.reshape(length, HEADS, 2, HD), (1, 0, 2, 3))
    value_heads = jnp.transpose(values.reshape(length, HEADS, VD), (1, 0, 2))
    mixed = lax.map(lambda parts: head_attention(parts[0], parts[1], parts[2], parts[3]), (query_heads, key_heads, value_heads, mix_lambda))
    spread = lax.optimization_barrier(jnp.mean(mixed * mixed, axis=-1, keepdims=True))
    normed = mixed * lax.rsqrt(spread + 1e-06) * head_gain * 0.8
    heads_out = jnp.transpose(normed, (1, 0, 2)).reshape(length, HEADS * VD).astype(jnp.bfloat16)
    after_mixer = resid.astype(jnp.float32) + jnp.dot(heads_out, out_weight, preferred_element_type=jnp.float32)
    squares = lax.optimization_barrier(jnp.mean(after_mixer * after_mixer, axis=-1, keepdims=True))
    normed_rows = (after_mixer * lax.rsqrt(squares + 1e-06) * norm_gain).astype(jnp.bfloat16)
    gated = jnp.dot(normed_rows, gate_weight, preferred_element_type=jnp.float32).astype(jnp.bfloat16)
    upward = jnp.dot(normed_rows, up_weight, preferred_element_type=jnp.float32)
    padded = jnp.pad(gated.astype(jnp.float32), ((1, 1), (0, 0)))
    conv = padded[:-2] * conv_weight[0] + padded[1:-1] * conv_weight[1] + padded[2:] * conv_weight[2] + conv_bias
    hidden = (jax.nn.silu(conv) * upward).astype(jnp.bfloat16)
    span = FF // N_TP
    hidden_blocks = jnp.transpose(hidden.reshape(length, N_TP, span), (1, 0, 2))
    down_blocks = down_weight.reshape(N_TP, span, D)

    def block_sum(carry, pair):
        part = jnp.dot(pair[0], pair[1], preferred_element_type=jnp.float32).astype(jnp.bfloat16)
        return (carry + part.astype(jnp.float32), None)
    mixer_out, unused = lax.scan(block_sum, jnp.zeros((length, D), jnp.float32), (hidden_blocks, down_blocks))
    return (after_mixer + mixer_out).astype(jnp.bfloat16)
```

```python
import functools
import math

import jax
import jax.numpy as jnp
from jax import lax
from jax.experimental import pallas as pl
from jax.experimental.pallas import tpu as pltpu
from jax.sharding import PartitionSpec as P

D = 2048
HD = 64
VD = 128


def with_halo(cells, sides, width):
    for axis, dim in sides:
        count = lax.axis_size(axis)
        ends = count - 1
        head = lax.slice_in_dim(cells, 0, width, axis=dim)
        tail = lax.slice_in_dim(cells, cells.shape[dim] - width, cells.shape[dim], axis=dim)
        cells = jnp.concatenate(
            [
                lax.ppermute(tail, axis, [(i, (i + 1) % count) for i in range(ends)]),
                cells,
                lax.ppermute(head, axis, [((i + 1) % count, i) for i in range(ends)]),
            ],
            axis=dim,
        )
    return cells


def on_device(
    resid,
    queries,
    keys,
    values,
    mix_lambda,
    head_gain,
    out_weight,
    norm_gain,
    gate_weight,
    up_weight,
    conv_weight,
    conv_bias,
    down_weight,
):
    length = queries.shape[0]
    heads = mix_lambda.shape[0]
    scale = HD ** (-0.5)
    query_heads = queries.reshape(length, heads, 2, HD)
    initial = (
        jnp.full((heads, 2, length), -1e30, jnp.float32),
        jnp.zeros((heads, 2, length), jnp.float32),
        jnp.zeros((heads, 2, length, VD), jnp.float32),
    )
    key_rows = lax.all_gather(keys, "sp", axis=0, tiled=True)
    value_rows = lax.all_gather(values, "sp", axis=0, tiled=True)
    count = key_rows.shape[0]
    block = math.gcd(count, 2048)
    key_blocks = key_rows.reshape(count // block, block, heads, 2, HD)
    value_blocks = value_rows.reshape(count // block, block, heads, VD)

    def advance(state, blocks):
        running, totals, weighted = state
        key_block, value_block = blocks
        scores = (
            jnp.einsum(
                "qhmd,khmd->hmqk", query_heads, key_block, preferred_element_type=jnp.float32
            )
            * scale
        )
        highest = jnp.maximum(running, jnp.max(scores, axis=-1))
        factor = jnp.exp(running - highest)
        shifted = jnp.exp(scores - highest[..., None])
        totals = totals * factor + jnp.sum(shifted, axis=-1)
        weighted = weighted * factor[..., None] + jnp.einsum(
            "hmqk,khe->hmqe",
            shifted.astype(jnp.bfloat16),
            value_block,
            preferred_element_type=jnp.float32,
        )
        return ((highest, totals, weighted), None)

    result, unused = lax.scan(advance, initial, (key_blocks, value_blocks))
    running, totals, weighted = result
    mapped = weighted / totals[..., None]
    mixed = mapped[:, 0] - mix_lambda[:, None, None] * mapped[:, 1]
    spread = jnp.mean(mixed * mixed, axis=-1, keepdims=True)
    normed = mixed * lax.rsqrt(spread + 1e-06) * head_gain * 0.8
    heads_out = jnp.transpose(normed, (1, 0, 2)).reshape(length, heads * VD).astype(jnp.bfloat16)
    projected = jnp.dot(
        lax.all_gather(heads_out, "tp", axis=1, tiled=True),
        out_weight,
        preferred_element_type=jnp.float32,
    )
    after_mixer = resid.astype(jnp.float32) + projected
    squares = lax.psum(jnp.sum(after_mixer * after_mixer, axis=1), "tp")
    normed_rows = (after_mixer * lax.rsqrt(squares / D + 1e-06)[:, None] * norm_gain).astype(
        jnp.bfloat16
    )
    full_rows = lax.all_gather(normed_rows, "tp", axis=1, tiled=True)
    gate_sum = jnp.dot(
        full_rows,
        lax.all_gather(gate_weight, "sp", axis=0, tiled=True),
        preferred_element_type=jnp.float32,
    )
    upward = jnp.dot(
        full_rows,
        lax.all_gather(up_weight, "sp", axis=0, tiled=True),
        preferred_element_type=jnp.float32,
    )
    gated = gate_sum.astype(jnp.bfloat16)
    padded = with_halo(gated, (("sp", 0),), 1).astype(jnp.float32)
    conv = (
        padded[:-2] * conv_weight[0]
        + padded[1:-1] * conv_weight[1]
        + padded[2:] * conv_weight[2]
        + conv_bias
    )
    hidden = (jax.nn.silu(conv) * upward).astype(jnp.bfloat16)
    partial_terms = jnp.dot(
        hidden,
        lax.all_gather(down_weight, "sp", axis=1, tiled=True),
        preferred_element_type=jnp.float32,
    )
    mixer_out = lax.psum_scatter(
        partial_terms.astype(jnp.bfloat16), "tp", scatter_dimension=1, tiled=True
    ).astype(jnp.float32)
    return (after_mixer + mixer_out).astype(jnp.bfloat16)


PAIR, LINE = 0, 1
EDGE = 16


def layer_kernel(
    sp,
    tp,
    resid,
    queries,
    keys,
    values,
    mix_lambda,
    head_gain,
    out_weight,
    norm_gain,
    gate_weight,
    up_weight,
    conv_weight,
    conv_bias,
    down_weight,
    out,
    kv,
    gates,
    ups,
    downs,
    peaks,
    totals,
    weighted,
    heads_all,
    after,
    square_all,
    rows_all,
    gate_acc,
    up_acc,
    hidden,
    partials,
    landed,
    local_sem,
    kv_send,
    kv_recv,
    w_send,
    w_recv,
    head_send,
    head_recv,
    square_send,
    square_recv,
    row_send,
    row_recv,
    edge_send,
    edge_recv,
    part_send,
    part_recv,
):
    bf16, f32 = jnp.bfloat16, jnp.float32
    me = lax.axis_index("sp")
    t = lax.axis_index("tp")
    nz = sp // 2
    z, y = me // 2, lax.rem(me, 2)
    length = queries.shape[0]
    heads = queries.shape[1] // VD
    half_k = gate_weight.shape[0] // 2
    half_f = down_weight.shape[0] // 2
    weights = (gates, ups, downs)

    local = [
        pltpu.make_async_copy(keys, kv.at[me, 0], local_sem.at[0]),
        pltpu.make_async_copy(values, kv.at[me, 1], local_sem.at[1]),
    ]
    for i, ref in enumerate((gate_weight, up_weight)):
        for h in range(2):
            local.append(
                pltpu.make_async_copy(
                    ref.at[pl.ds(h * half_k, half_k)],
                    weights[i].at[me, h],
                    local_sem.at[2 + 2 * i + h],
                )
            )
    for h in range(2):
        local.append(
            pltpu.make_async_copy(
                down_weight.at[pl.ds(h * half_f, half_f)], downs.at[me, h], local_sem.at[6 + h]
            )
        )
    for copy in local:
        copy.start()

    def routes(kind, zs, ys):
        if kind == PAIR:
            up = jnp.logical_and(zs <= z, z < nz - 1)
            down = jnp.logical_and(zs >= z, z > 0)
            across = jnp.logical_and(zs == z, ys == y)
        else:
            up = jnp.logical_and(ys == y, jnp.logical_and(zs <= z, z < nz - 1))
            down = jnp.logical_and(ys == y, jnp.logical_and(zs >= z, z > 0))
            across = ys == y
        return (
            (up, jnp.minimum(me + 2, sp - 1)),
            (down, jnp.maximum(me - 2, 0)),
            (across, 2 * z + 1 - y),
        )

    def remote(ref, send, recv, target):
        return pltpu.make_async_remote_copy(
            src_ref=ref,
            dst_ref=ref,
            send_sem=send,
            recv_sem=recv,
            device_id={"sp": target},
            device_id_type=pl.DeviceIdType.MESH,
        )

    def kv_copy(kind, src, way, target):
        return remote(kv.at[src, kind], kv_send.at[kind, way, src], kv_recv.at[kind, src], target)

    def w_copy(array, kind, src, way, target):
        return remote(
            weights[array].at[src, kind],
            w_send.at[array, kind, way, src],
            w_recv.at[array, kind, src],
            target,
        )

    def push(make, kind, src, ways=(0, 1, 2), wait=False):
        zs, ys = src // 2, lax.rem(src, 2)
        plan = routes(kind, zs, ys)
        for way in ways:
            needed, target = plan[way]

            @pl.when(needed)
            def _():
                copy = make(kind, src, way, target)
                if wait:
                    copy.wait_send()
                else:
                    copy.start()

    def take(make, kind, src):
        @pl.when(src != me)
        def _():
            make(kind, src, 0, lax.rem(me + 2, sp)).wait_recv()
            push(make, kind, src)

    def visit(body, after_ring=None):
        def event(e, carry):
            d = e // 4
            above = lax.rem(e // 2, 2)
            ys = lax.rem(y + lax.rem(e, 2), 2)
            zs = jnp.where(above == 1, z + d, z - d)
            valid = jnp.logical_and(jnp.logical_and(zs >= 0, zs < nz), d + (1 - above) > 0)

            @pl.when(valid)
            def _():
                body(2 * zs + ys)

            if after_ring is not None:

                @pl.when(lax.rem(e, 4) == 3)
                def _():
                    after_ring(d)

            return carry

        lax.fori_loop(0, 4 * nz, event, 0)

    for copy in local:
        copy.wait()
    push(kv_copy, PAIR, me)
    push(kv_copy, LINE, me)

    peaks[...] = jnp.full(peaks.shape, -1e30, f32)
    totals[...] = jnp.zeros(totals.shape, f32)
    weighted[...] = jnp.zeros(weighted.shape, f32)
    lanes = lax.broadcasted_iota(jnp.int32, (1, 2 * HD), 1)
    scale = HD**-0.5
    rows = math.gcd(length, 256)

    def attend(src):
        take(kv_copy, PAIR, src)
        take(kv_copy, LINE, src)

        def row_block(r, carry):
            at = pl.ds(pl.multiple_of(r * rows, rows), rows)
            for h in range(heads):
                cols = slice(h * VD, (h + 1) * VD)
                q = queries[at, cols].astype(f32) * scale
                key_block = kv[src, 0, :, cols]
                value_block = kv[src, 1, :, cols]
                for m in range(2):
                    keep = lanes < HD if m == 0 else lanes >= HD
                    qm = jnp.where(keep, q, 0.0).astype(bf16)
                    s = lax.dot_general(
                        qm, key_block, (((1,), (1,)), ((), ())), preferred_element_type=f32
                    )
                    i = 2 * h + m
                    old = peaks[i, at, :]
                    new = jnp.maximum(old, jnp.max(s, axis=1, keepdims=True))
                    factor = jnp.exp(old - new)
                    p = jnp.exp(s - new)
                    peaks[i, at, :] = new
                    totals[i, at, :] = totals[i, at, :] * factor + jnp.sum(
                        p, axis=1, keepdims=True
                    )
                    weighted[i, at, :] = weighted[i, at, :] * factor + jnp.dot(
                        p.astype(bf16), value_block, preferred_element_type=f32
                    )
            return carry

        lax.fori_loop(0, length // rows, row_block, 0)

    def feed(d):
        for way, turn in ((0, z), (1, nz - 1 - z), (2, nz - 1)):

            @pl.when(d == turn)
            def _():
                for array in range(3):
                    for kind in (PAIR, LINE):
                        push(functools.partial(w_copy, array), kind, me, (way,))

    visit(attend, feed)

    for h in range(heads):
        first = weighted[2 * h] / totals[2 * h]
        second = weighted[2 * h + 1] / totals[2 * h + 1]
        mixed = first - mix_lambda[h] * second
        spread = jnp.mean(mixed * mixed, axis=1, keepdims=True)
        normed = mixed * lax.rsqrt(spread + 1e-06) * head_gain[...] * 0.8
        heads_all[t, :, h * VD : (h + 1) * VD] = normed.astype(bf16)

    def to_peers(ref_of, send, recv):
        copies = []
        for j in range(1, tp):
            copy = pltpu.make_async_remote_copy(
                src_ref=ref_of,
                dst_ref=ref_of,
                send_sem=send.at[j],
                recv_sem=recv.at[j],
                device_id={"tp": lax.rem(t + j, tp)},
                device_id_type=pl.DeviceIdType.MESH,
            )
            copy.start()
            copies.append(copy)
        return copies

    sent = to_peers(heads_all.at[t], head_send, head_recv)
    for copy in sent:
        copy.wait()
    width = heads * VD
    total = resid[...].astype(f32)
    for j in range(tp):
        total = total + jnp.dot(
            heads_all[j], out_weight[j * width : (j + 1) * width, :], preferred_element_type=f32
        )
    after[...] = total
    row_sum = jnp.sum(total * total, axis=1, keepdims=True)
    square_all[t] = jnp.transpose(jnp.broadcast_to(row_sum, (length, 128)))[:8]
    sent = to_peers(square_all.at[t], square_send, square_recv)
    for copy in sent:
        copy.wait()
    summed = square_all[0]
    for j in range(1, tp):
        summed = summed + square_all[j]
    inverse = lax.rsqrt(summed / D + 1e-06)
    inverse = jnp.transpose(jnp.concatenate([inverse] * 16, axis=0))[:, :1]
    rows_all[t, EDGE : EDGE + length, :] = (after[...] * inverse * norm_gain[...]).astype(bf16)
    sent = to_peers(rows_all.at[t, pl.ds(EDGE, length)], row_send, row_recv)
    for copy in sent:
        copy.wait()

    def edge_copy(way, source, dest, target):
        return pltpu.make_async_remote_copy(
            src_ref=rows_all.at[:, pl.ds(source, EDGE)],
            dst_ref=rows_all.at[:, pl.ds(dest, EDGE)],
            send_sem=edge_send.at[way],
            recv_sem=edge_recv.at[way],
            device_id={"sp": target},
            device_id_type=pl.DeviceIdType.MESH,
        )

    onward = edge_copy(0, length, 0, jnp.minimum(me + 1, sp - 1))
    back = edge_copy(1, EDGE, EDGE + length, jnp.maximum(me - 1, 0))
    not_last, not_first = me < sp - 1, me > 0

    @pl.when(not_last)
    def _():
        onward.start()

    @pl.when(not_first)
    def _():
        back.start()

    @pl.when(me == 0)
    def _():
        rows_all[:, 0:EDGE, :] = jnp.zeros((tp, EDGE, rows_all.shape[2]), bf16)

    @pl.when(me == sp - 1)
    def _():
        rows_all[:, EDGE + length :, :] = jnp.zeros((tp, EDGE, rows_all.shape[2]), bf16)

    @pl.when(not_first)
    def _():
        onward.wait_recv()

    @pl.when(not_last)
    def _():
        back.wait_recv()

    gate_acc[...] = jnp.zeros(gate_acc.shape, f32)
    up_acc[...] = jnp.zeros(up_acc.shape, f32)
    per = sp // tp
    depth = 2 * half_k
    ff = gate_weight.shape[1]

    def expand(src):
        for array in range(2):
            for kind in (PAIR, LINE):
                take(functools.partial(w_copy, array), kind, src)
        cols = pl.ds(pl.multiple_of(lax.rem(src, per) * depth, depth), depth)
        x = rows_all[src // per, :, cols]
        gate_acc[...] += jnp.dot(
            x, gates[src].reshape(depth, ff), preferred_element_type=f32
        )
        up_acc[...] += jnp.dot(
            x[EDGE : EDGE + length], ups[src].reshape(depth, ff), preferred_element_type=f32
        )

    visit(expand)

    for c in range(0, ff, 128):
        cols = slice(c, c + 128)

        def tap(start):
            return gate_acc[start : start + length, cols].astype(bf16).astype(f32)

        conv = (
            tap(EDGE - 1) * conv_weight[0:1, cols]
            + tap(EDGE) * conv_weight[1:2, cols]
            + tap(EDGE + 1) * conv_weight[2:3, cols]
            + conv_bias[:, cols]
        )
        hidden[:, cols] = (conv / (1.0 + jnp.exp(-conv)) * up_acc[:, cols]).astype(bf16)

    def part_copy(src, owner, sender):
        return pltpu.make_async_remote_copy(
            src_ref=partials.at[src],
            dst_ref=landed.at[sender, lax.rem(src, per)],
            send_sem=part_send.at[src],
            recv_sem=part_recv.at[sender, lax.rem(src, per)],
            device_id={"tp": owner},
            device_id_type=pl.DeviceIdType.MESH,
        )

    def contract(src):
        for kind in (PAIR, LINE):
            take(functools.partial(w_copy, 2), kind, src)
        part = jnp.dot(
            hidden[...],
            downs[src].reshape(2 * half_f, downs.shape[3]),
            preferred_element_type=f32,
        )
        partials[src] = part.astype(bf16)
        owner = src // per

        @pl.when(owner != t)
        def _():
            part_copy(src, owner, t).start()

    visit(contract)

    wide = partials.shape[2]
    for q in range(per):
        cols = slice(q * wide, (q + 1) * wide)
        total = partials[t * per + q].astype(f32)
        for j in range(1, tp):
            sender = lax.rem(t + j, tp)
            part_copy(t * per + q, sender, sender).wait_recv()
            total = total + landed[sender, q].astype(f32)
        out[:, cols] = (after[:, cols] + total).astype(bf16)

    @pl.when(not_last)
    def _():
        onward.wait_send()

    @pl.when(not_first)
    def _():
        back.wait_send()

    def drain(src, carry):
        for kind in (PAIR, LINE):
            push(kv_copy, kind, src, wait=True)
            for array in range(3):
                push(functools.partial(w_copy, array), kind, src, wait=True)

        @pl.when(src // per != t)
        def _():
            part_copy(src, src // per, t).wait_send()

        return carry

    lax.fori_loop(0, sp, drain, 0)


def fused(sp, tp, *args):
    resid, queries, keys, values = args[:4]
    gate_weight, down_weight = args[8], args[12]
    length, width = queries.shape
    features = resid.shape[1]
    depth, ff = gate_weight.shape
    maps = 2 * (width // VD)
    bf16, f32 = jnp.bfloat16, jnp.float32
    dma = pltpu.SemaphoreType.DMA
    vmem = pl.BlockSpec(memory_space=pltpu.VMEM)
    smem = pl.BlockSpec(memory_space=pltpu.SMEM)
    hbm = pl.BlockSpec(memory_space=pl.ANY)
    rows = length + 2 * EDGE
    down_cols = down_weight.shape[1]
    args = list(args)
    for i in (5, 7, 11):
        args[i] = args[i].reshape(1, -1)
    return pl.pallas_call(
        functools.partial(layer_kernel, sp, tp),
        out_shape=jax.ShapeDtypeStruct(resid.shape, bf16),
        in_specs=[
            vmem, vmem, hbm, hbm, smem, vmem, vmem, vmem, hbm, hbm, vmem, vmem, hbm,
        ],
        out_specs=vmem,
        scratch_shapes=[
            pltpu.VMEM((sp, 2, length, width), bf16),
            pltpu.VMEM((sp, 2, depth // 2, ff), bf16),
            pltpu.VMEM((sp, 2, depth // 2, ff), bf16),
            pltpu.VMEM((sp, 2, ff // 2, down_cols), bf16),
            pltpu.VMEM((maps, length, 1), f32),
            pltpu.VMEM((maps, length, 1), f32),
            pltpu.VMEM((maps, length, VD), f32),
            pltpu.VMEM((tp, length, width), bf16),
            pltpu.VMEM((length, features), f32),
            pltpu.VMEM((tp, 8, length), f32),
            pltpu.VMEM((tp, rows, features), bf16),
            pltpu.VMEM((rows, ff), f32),
            pltpu.VMEM((length, ff), f32),
            pltpu.VMEM((length, ff), bf16),
            pltpu.VMEM((sp, length, down_cols), bf16),
            pltpu.VMEM((tp, sp // tp, length, down_cols), bf16),
            dma((8,)),
            dma((2, 3, sp)),
            dma((2, sp)),
            dma((3, 2, 3, sp)),
            dma((3, 2, sp)),
            dma((tp,)),
            dma((tp,)),
            dma((tp,)),
            dma((tp,)),
            dma((tp,)),
            dma((tp,)),
            dma((2,)),
            dma((2,)),
            dma((sp,)),
            dma((tp, sp // tp)),
        ],
        compiler_params=pltpu.CompilerParams(
            has_side_effects=True, vmem_limit_bytes=60 * 1024 * 1024
        ),
    )(*args)


def solution(mesh):
    sp, tp = mesh.shape["sp"], mesh.shape["tp"]

    def run(*args):
        width, depth = args[1].shape[1], args[8].shape[0]
        small = args[0].shape[0] <= 512
        whole_pairs = sp % 2 == 0 and sp % tp == 0
        if whole_pairs and small and depth % 256 == 0 and width % VD == 0:
            return fused(sp, tp, *args)
        return on_device(*args)


    placed = (
        P("sp", "tp"),
        P("sp", "tp"),
        P("sp", "tp"),
        P("sp", "tp"),
        P("tp"),
        P(),
        P(None, "tp"),
        P("tp"),
        P("sp", "tp"),
        P("sp", "tp"),
        P(None, "tp"),
        P("tp"),
        P("tp", "sp"),
    )
    return jax.shard_map(
        run, mesh=mesh, in_specs=placed, out_specs=P("sp", "tp"), check_vma=False
    )
```

```python
import functools
import math

import jax
import jax.numpy as jnp
from jax import lax
from jax.experimental import pallas as pl
from jax.experimental.pallas import tpu as pltpu
from jax.sharding import PartitionSpec as P

D = 2048
HD = 64
VD = 128


def with_halo(cells, sides, width):
    for axis, dim in sides:
        count = lax.axis_size(axis)
        ends = count - 1
        head = lax.slice_in_dim(cells, 0, width, axis=dim)
        tail = lax.slice_in_dim(cells, cells.shape[dim] - width, cells.shape[dim], axis=dim)
        cells = jnp.concatenate(
            [
                lax.ppermute(tail, axis, [(i, (i + 1) % count) for i in range(ends)]),
                cells,
                lax.ppermute(head, axis, [((i + 1) % count, i) for i in range(ends)]),
            ],
            axis=dim,
        )
    return cells


def on_device(
    resid,
    queries,
    keys,
    values,
    mix_lambda,
    head_gain,
    out_weight,
    norm_gain,
    gate_weight,
    up_weight,
    conv_weight,
    conv_bias,
    down_weight,
):
    length = queries.shape[0]
    heads = mix_lambda.shape[0]
    scale = HD ** (-0.5)
    query_heads = queries.reshape(length, heads, 2, HD)
    initial = (
        jnp.full((heads, 2, length), -1e30, jnp.float32),
        jnp.zeros((heads, 2, length), jnp.float32),
        jnp.zeros((heads, 2, length, VD), jnp.float32),
    )
    key_rows = lax.all_gather(keys, "sp", axis=0, tiled=True)
    value_rows = lax.all_gather(values, "sp", axis=0, tiled=True)
    count = key_rows.shape[0]
    block = math.gcd(count, 2048)
    key_blocks = key_rows.reshape(count // block, block, heads, 2, HD)
    value_blocks = value_rows.reshape(count // block, block, heads, VD)

    def advance(state, blocks):
        running, totals, weighted = state
        key_block, value_block = blocks
        scores = (
            jnp.einsum(
                "qhmd,khmd->hmqk", query_heads, key_block, preferred_element_type=jnp.float32
            )
            * scale
        )
        highest = jnp.maximum(running, jnp.max(scores, axis=-1))
        factor = jnp.exp(running - highest)
        shifted = jnp.exp(scores - highest[..., None])
        totals = totals * factor + jnp.sum(shifted, axis=-1)
        weighted = weighted * factor[..., None] + jnp.einsum(
            "hmqk,khe->hmqe",
            shifted.astype(jnp.bfloat16),
            value_block,
            preferred_element_type=jnp.float32,
        )
        return ((highest, totals, weighted), None)

    result, unused = lax.scan(advance, initial, (key_blocks, value_blocks))
    running, totals, weighted = result
    mapped = weighted / totals[..., None]
    mixed = mapped[:, 0] - mix_lambda[:, None, None] * mapped[:, 1]
    spread = jnp.mean(mixed * mixed, axis=-1, keepdims=True)
    normed = mixed * lax.rsqrt(spread + 1e-06) * head_gain * 0.8
    heads_out = jnp.transpose(normed, (1, 0, 2)).reshape(length, heads * VD).astype(jnp.bfloat16)
    projected = jnp.dot(
        lax.all_gather(heads_out, "tp", axis=1, tiled=True),
        out_weight,
        preferred_element_type=jnp.float32,
    )
    after_mixer = resid.astype(jnp.float32) + projected
    squares = lax.psum(jnp.sum(after_mixer * after_mixer, axis=1), "tp")
    normed_rows = (after_mixer * lax.rsqrt(squares / D + 1e-06)[:, None] * norm_gain).astype(
        jnp.bfloat16
    )
    full_rows = lax.all_gather(normed_rows, "tp", axis=1, tiled=True)
    gate_sum = jnp.dot(
        full_rows,
        lax.all_gather(gate_weight, "sp", axis=0, tiled=True),
        preferred_element_type=jnp.float32,
    )
    upward = jnp.dot(
        full_rows,
        lax.all_gather(up_weight, "sp", axis=0, tiled=True),
        preferred_element_type=jnp.float32,
    )
    gated = gate_sum.astype(jnp.bfloat16)
    padded = with_halo(gated, (("sp", 0),), 1).astype(jnp.float32)
    conv = (
        padded[:-2] * conv_weight[0]
        + padded[1:-1] * conv_weight[1]
        + padded[2:] * conv_weight[2]
        + conv_bias
    )
    hidden = (jax.nn.silu(conv) * upward).astype(jnp.bfloat16)
    partial_terms = jnp.dot(
        hidden,
        lax.all_gather(down_weight, "sp", axis=1, tiled=True),
        preferred_element_type=jnp.float32,
    )
    mixer_out = lax.psum_scatter(
        partial_terms.astype(jnp.bfloat16), "tp", scatter_dimension=1, tiled=True
    ).astype(jnp.float32)
    return (after_mixer + mixer_out).astype(jnp.bfloat16)


PAIR, LINE = 0, 1
EDGE = 16


def layer_kernel(
    sp,
    tp,
    resid,
    queries,
    keys,
    values,
    mix_lambda,
    head_gain,
    out_weight,
    norm_gain,
    gate_weight,
    up_weight,
    conv_weight,
    conv_bias,
    down_weight,
    out,
    kv,
    gates,
    ups,
    downs,
    peaks,
    totals,
    weighted,
    heads_all,
    after,
    square_all,
    rows_all,
    gate_acc,
    up_acc,
    hidden,
    partials,
    landed,
    local_sem,
    kv_send,
    kv_recv,
    w_send,
    w_recv,
    head_send,
    head_recv,
    square_send,
    square_recv,
    row_send,
    row_recv,
    edge_send,
    edge_recv,
    part_send,
    part_recv,
):
    bf16, f32 = jnp.bfloat16, jnp.float32
    me = lax.axis_index("sp")
    t = lax.axis_index("tp")
    nz = sp // 2
    z, y = me // 2, lax.rem(me, 2)
    length = queries.shape[0]
    heads = queries.shape[1] // VD
    half_k = gate_weight.shape[0] // 2
    half_f = down_weight.shape[0] // 2
    weights = (gates, ups, downs)

    local = [
        pltpu.make_async_copy(keys, kv.at[me, 0], local_sem.at[0]),
        pltpu.make_async_copy(values, kv.at[me, 1], local_sem.at[1]),
    ]
    for i, ref in enumerate((gate_weight, up_weight)):
        for h in range(2):
            local.append(
                pltpu.make_async_copy(
                    ref.at[pl.ds(h * half_k, half_k)],
                    weights[i].at[me, h],
                    local_sem.at[2 + 2 * i + h],
                )
            )
    for h in range(2):
        local.append(
            pltpu.make_async_copy(
                down_weight.at[pl.ds(h * half_f, half_f)], downs.at[me, h], local_sem.at[6 + h]
            )
        )
    for copy in local:
        copy.start()

    def routes(kind, zs, ys):
        if kind == PAIR:
            up = jnp.logical_and(zs <= z, z < nz - 1)
            down = jnp.logical_and(zs >= z, z > 0)
            across = jnp.logical_and(zs == z, ys == y)
        else:
            up = jnp.logical_and(ys == y, jnp.logical_and(zs <= z, z < nz - 1))
            down = jnp.logical_and(ys == y, jnp.logical_and(zs >= z, z > 0))
            across = ys == y
        return (
            (up, jnp.minimum(me + 2, sp - 1)),
            (down, jnp.maximum(me - 2, 0)),
            (across, 2 * z + 1 - y),
        )

    def remote(ref, send, recv, target):
        return pltpu.make_async_remote_copy(
            src_ref=ref,
            dst_ref=ref,
            send_sem=send,
            recv_sem=recv,
            device_id={"sp": target},
            device_id_type=pl.DeviceIdType.MESH,
        )

    def kv_copy(kind, src, way, target):
        return remote(kv.at[src, kind], kv_send.at[kind, way, src], kv_recv.at[kind, src], target)

    def w_copy(array, kind, src, way, target):
        return remote(
            weights[array].at[src, kind],
            w_send.at[array, kind, way, src],
            w_recv.at[array, kind, src],
            target,
        )

    def push(make, kind, src, ways=(0, 1, 2), wait=False):
        zs, ys = src // 2, lax.rem(src, 2)
        plan = routes(kind, zs, ys)
        for way in ways:
            needed, target = plan[way]

            @pl.when(needed)
            def _():
                copy = make(kind, src, way, target)
                if wait:
                    copy.wait_send()
                else:
                    copy.start()

    def take(make, kind, src):
        @pl.when(src != me)
        def _():
            make(kind, src, 0, lax.rem(me + 2, sp)).wait_recv()
            push(make, kind, src)

    def visit(first, last, body, after_ring=None):
        def event(e, carry):
            d = e // 4
            above = lax.rem(e, 2)
            ys = lax.rem(y + lax.rem(e // 2, 2), 2)
            zs = jnp.where(above == 1, z + d, z - d)
            valid = jnp.logical_and(jnp.logical_and(zs >= 0, zs < nz), d + (1 - above) > 0)

            @pl.when(valid)
            def _():
                body(2 * zs + ys)

            if after_ring is not None:

                @pl.when(lax.rem(e, 4) == 3)
                def _():
                    after_ring(d)

            return carry

        lax.fori_loop(4 * first, 4 * last, event, 0)

    for copy in local:
        copy.wait()
    push(kv_copy, PAIR, me)
    push(kv_copy, LINE, me)

    peaks[...] = jnp.full(peaks.shape, -1e30, f32)
    totals[...] = jnp.zeros(totals.shape, f32)
    weighted[...] = jnp.zeros(weighted.shape, f32)
    lanes = lax.broadcasted_iota(jnp.int32, (1, 2 * HD), 1)
    scale = HD**-0.5
    rows = math.gcd(length, 256)

    def attend(src):
        take(kv_copy, PAIR, src)
        take(kv_copy, LINE, src)

        def row_block(r, carry):
            at = pl.ds(pl.multiple_of(r * rows, rows), rows)
            for h in range(heads):
                cols = slice(h * VD, (h + 1) * VD)
                q = queries[at, cols].astype(f32) * scale
                key_block = kv[src, 0, :, cols]
                value_block = kv[src, 1, :, cols]
                for m in range(2):
                    keep = lanes < HD if m == 0 else lanes >= HD
                    qm = jnp.where(keep, q, 0.0).astype(bf16)
                    s = lax.dot_general(
                        qm, key_block, (((1,), (1,)), ((), ())), preferred_element_type=f32
                    )
                    i = 2 * h + m
                    old = peaks[i, at, :]
                    new = jnp.maximum(old, jnp.max(s, axis=1, keepdims=True))
                    factor = jnp.exp(old - new)
                    p = jnp.exp(s - new)
                    peaks[i, at, :] = new
                    totals[i, at, :] = totals[i, at, :] * factor + jnp.sum(
                        p, axis=1, keepdims=True
                    )
                    weighted[i, at, :] = weighted[i, at, :] * factor + jnp.dot(
                        p.astype(bf16), value_block, preferred_element_type=f32
                    )
            return carry

        lax.fori_loop(0, length // rows, row_block, 0)

    def feed(d):
        for way, turn in ((0, z), (1, nz - 1 - z), (2, nz - 1)):

            @pl.when(d == turn)
            def _():
                for array in range(3):
                    for kind in (PAIR, LINE):
                        push(functools.partial(w_copy, array), kind, me, (way,))

    visit(0, nz, attend, feed)

    for h in range(heads):
        first = weighted[2 * h] / totals[2 * h]
        second = weighted[2 * h + 1] / totals[2 * h + 1]
        mixed = first - mix_lambda[h] * second
        spread = jnp.mean(mixed * mixed, axis=1, keepdims=True)
        normed = mixed * lax.rsqrt(spread + 1e-06) * head_gain[...] * 0.8
        heads_all[t, :, h * VD : (h + 1) * VD] = normed.astype(bf16)

    core = lax.rem(t, 2)
    sibling = t + 1 - 2 * core
    half_tp = tp // 2

    def tp_copy(ref, send, recv, target):
        return pltpu.make_async_remote_copy(
            src_ref=ref,
            dst_ref=ref,
            send_sem=send,
            recv_sem=recv,
            device_id={"tp": target},
            device_id_type=pl.DeviceIdType.MESH,
        )

    def spread(slot, send, recv):
        copies = []
        for k in range(1, half_tp):
            copies.append(tp_copy(slot(t), send.at[k], recv.at[k], lax.rem(t + 2 * k, tp)))
            copies[-1].start()
        copies.append(tp_copy(slot(t), send.at[0], recv.at[0], sibling))
        copies[-1].start()
        return copies

    def settle(slot, send, recv, copies):
        for k in range(1, half_tp):
            copies[k - 1].wait_recv()
            came = lax.rem(t + tp - 2 * k, tp)
            copies.append(
                tp_copy(slot(came), send.at[half_tp + k], recv.at[half_tp + k], sibling)
            )
            copies[-1].start()
        for copy in copies[half_tp - 1 :]:
            copy.wait_recv()
        for copy in copies:
            copy.wait_send()

    def exchange(slot, send, recv):
        settle(slot, send, recv, spread(slot, send, recv))

    exchange(lambda j: heads_all.at[j], head_send, head_recv)
    width = heads * VD
    total = resid[...].astype(f32)
    for j in range(tp):
        total = total + jnp.dot(
            heads_all[j], out_weight[j * width : (j + 1) * width, :], preferred_element_type=f32
        )
    after[...] = total
    row_sum = jnp.sum(total * total, axis=1, keepdims=True)
    square_all[t] = jnp.transpose(jnp.broadcast_to(row_sum, (length, 128)))[:8]
    exchange(lambda j: square_all.at[j], square_send, square_recv)
    summed = square_all[0]
    for j in range(1, tp):
        summed = summed + square_all[j]
    inverse = lax.rsqrt(summed / D + 1e-06)
    inverse = jnp.transpose(jnp.concatenate([inverse] * 16, axis=0))[:, :1]
    rows_all[t, EDGE : EDGE + length, :] = (after[...] * inverse * norm_gain[...]).astype(bf16)
    own_rows = lambda j: rows_all.at[j, pl.ds(EDGE, length)]
    sent = spread(own_rows, row_send, row_recv)

    def relay(src):
        for array in range(3):
            for kind in (PAIR, LINE):
                take(functools.partial(w_copy, array), kind, src)

    visit(0, 1, relay)
    settle(own_rows, row_send, row_recv, sent)

    def edge_copy(way, source, dest, target):
        return pltpu.make_async_remote_copy(
            src_ref=rows_all.at[:, pl.ds(source, EDGE)],
            dst_ref=rows_all.at[:, pl.ds(dest, EDGE)],
            send_sem=edge_send.at[way],
            recv_sem=edge_recv.at[way],
            device_id={"sp": target},
            device_id_type=pl.DeviceIdType.MESH,
        )

    onward = edge_copy(0, length, 0, jnp.minimum(me + 1, sp - 1))
    back = edge_copy(1, EDGE, EDGE + length, jnp.maximum(me - 1, 0))
    not_last, not_first = me < sp - 1, me > 0

    @pl.when(not_last)
    def _():
        onward.start()

    @pl.when(not_first)
    def _():
        back.start()

    @pl.when(me == 0)
    def _():
        rows_all[:, 0:EDGE, :] = jnp.zeros((tp, EDGE, rows_all.shape[2]), bf16)

    @pl.when(me == sp - 1)
    def _():
        rows_all[:, EDGE + length :, :] = jnp.zeros((tp, EDGE, rows_all.shape[2]), bf16)

    visit(1, 2, relay)

    @pl.when(not_first)
    def _():
        onward.wait_recv()

    @pl.when(not_last)
    def _():
        back.wait_recv()

    gate_acc[...] = jnp.zeros(gate_acc.shape, f32)
    up_acc[...] = jnp.zeros(up_acc.shape, f32)
    per = sp // tp
    depth = 2 * half_k
    ff = gate_weight.shape[1]

    def expand(src):
        cols = pl.ds(pl.multiple_of(lax.rem(src, per) * depth, depth), depth)
        x = rows_all[src // per, :, cols]
        gate_acc[...] += jnp.dot(
            x, gates[src].reshape(depth, ff), preferred_element_type=f32
        )
        up_acc[...] += jnp.dot(
            x[EDGE : EDGE + length], ups[src].reshape(depth, ff), preferred_element_type=f32
        )

    def relay_expand(src):
        relay(src)
        expand(src)

    visit(0, 2, expand)
    visit(2, nz, relay_expand)

    for c in range(0, ff, 128):
        cols = slice(c, c + 128)

        def tap(start):
            return gate_acc[start : start + length, cols].astype(bf16).astype(f32)

        conv = (
            tap(EDGE - 1) * conv_weight[0:1, cols]
            + tap(EDGE) * conv_weight[1:2, cols]
            + tap(EDGE + 1) * conv_weight[2:3, cols]
            + conv_bias[:, cols]
        )
        hidden[:, cols] = (conv / (1.0 + jnp.exp(-conv)) * up_acc[:, cols]).astype(bf16)

    def part(owner, q):
        return jnp.dot(
            hidden[...],
            downs[owner * per + q].reshape(2 * half_f, downs.shape[3]),
            preferred_element_type=f32,
        )

    def part_copy(slot, q, target):
        return pltpu.make_async_remote_copy(
            src_ref=partials.at[slot, q],
            dst_ref=landed.at[slot, q],
            send_sem=part_send.at[slot, q],
            recv_sem=part_recv.at[slot, q],
            device_id={"tp": target},
            device_id_type=pl.DeviceIdType.MESH,
        )

    shipped = []
    for k in range(1, half_tp):
        chip = lax.rem(t // 2 + k, half_tp)
        for q in range(per):
            partials[half_tp + k, q] = part(2 * chip + 1 - core, q).astype(bf16)
            copy = part_copy(half_tp + k, q, sibling)
            copy.start()
            shipped.append(copy)
        for q in range(per):
            mine = part(2 * chip + core, q)
            shipped[(k - 1) * 2 * per + q].wait_recv()
            partials[k, q] = (mine + landed[half_tp + k, q].astype(f32)).astype(bf16)
            copy = part_copy(k, q, 2 * chip + core)
            copy.start()
            shipped.append(copy)
    for q in range(per):
        partials[0, q] = part(sibling, q).astype(bf16)
        copy = part_copy(0, q, sibling)
        copy.start()
        shipped.append(copy)
    wide = partials.shape[3]
    for q in range(per):
        cols = slice(q * wide, (q + 1) * wide)
        after[:, cols] += part(t, q)
    for q in range(per):
        cols = slice(q * wide, (q + 1) * wide)
        total = after[:, cols]
        for k in range(half_tp):
            part_copy(k, q, sibling).wait_recv()
            total = total + landed[k, q].astype(f32)
        out[:, cols] = total.astype(bf16)
    for copy in shipped:
        copy.wait_send()

    @pl.when(not_last)
    def _():
        onward.wait_send()

    @pl.when(not_first)
    def _():
        back.wait_send()

    def drain(src, carry):
        for kind in (PAIR, LINE):
            push(kv_copy, kind, src, wait=True)
            for array in range(3):
                push(functools.partial(w_copy, array), kind, src, wait=True)

        return carry

    lax.fori_loop(0, sp, drain, 0)


def fused(sp, tp, *args):
    resid, queries, keys, values = args[:4]
    gate_weight, down_weight = args[8], args[12]
    length, width = queries.shape
    features = resid.shape[1]
    depth, ff = gate_weight.shape
    maps = 2 * (width // VD)
    bf16, f32 = jnp.bfloat16, jnp.float32
    dma = pltpu.SemaphoreType.DMA
    vmem = pl.BlockSpec(memory_space=pltpu.VMEM)
    smem = pl.BlockSpec(memory_space=pltpu.SMEM)
    hbm = pl.BlockSpec(memory_space=pl.ANY)
    rows = length + 2 * EDGE
    down_cols = down_weight.shape[1]
    args = list(args)
    for i in (5, 7, 11):
        args[i] = args[i].reshape(1, -1)
    return pl.pallas_call(
        functools.partial(layer_kernel, sp, tp),
        out_shape=jax.ShapeDtypeStruct(resid.shape, bf16),
        in_specs=[
            vmem, vmem, hbm, hbm, smem, vmem, vmem, vmem, hbm, hbm, vmem, vmem, hbm,
        ],
        out_specs=vmem,
        scratch_shapes=[
            pltpu.VMEM((sp, 2, length, width), bf16),
            pltpu.VMEM((sp, 2, depth // 2, ff), bf16),
            pltpu.VMEM((sp, 2, depth // 2, ff), bf16),
            pltpu.VMEM((sp, 2, ff // 2, down_cols), bf16),
            pltpu.VMEM((maps, length, 1), f32),
            pltpu.VMEM((maps, length, 1), f32),
            pltpu.VMEM((maps, length, VD), f32),
            pltpu.VMEM((tp, length, width), bf16),
            pltpu.VMEM((length, features), f32),
            pltpu.VMEM((tp, 8, length), f32),
            pltpu.VMEM((tp, rows, features), bf16),
            pltpu.VMEM((rows, ff), f32),
            pltpu.VMEM((length, ff), f32),
            pltpu.VMEM((length, ff), bf16),
            pltpu.VMEM((tp, sp // tp, length, down_cols), bf16),
            pltpu.VMEM((tp, sp // tp, length, down_cols), bf16),
            dma((8,)),
            dma((2, 3, sp)),
            dma((2, sp)),
            dma((3, 2, 3, sp)),
            dma((3, 2, sp)),
            dma((tp,)),
            dma((tp,)),
            dma((tp,)),
            dma((tp,)),
            dma((tp,)),
            dma((tp,)),
            dma((2,)),
            dma((2,)),
            dma((tp, sp // tp)),
            dma((tp, sp // tp)),
        ],
        compiler_params=pltpu.CompilerParams(
            has_side_effects=True, vmem_limit_bytes=60 * 1024 * 1024
        ),
    )(*args)


def solution(mesh):
    sp, tp = mesh.shape["sp"], mesh.shape["tp"]

    def run(*args):
        width, depth = args[1].shape[1], args[8].shape[0]
        small = args[0].shape[0] <= 512
        whole_pairs = sp % 2 == 0 and tp % 2 == 0 and sp % tp == 0
        if whole_pairs and small and depth % 256 == 0 and width % VD == 0:
            return fused(sp, tp, *args)
        return on_device(*args)


    placed = (
        P("sp", "tp"),
        P("sp", "tp"),
        P("sp", "tp"),
        P("sp", "tp"),
        P("tp"),
        P(),
        P(None, "tp"),
        P("tp"),
        P("sp", "tp"),
        P("sp", "tp"),
        P(None, "tp"),
        P("tp"),
        P("tp", "sp"),
    )
    return jax.shard_map(
        run, mesh=mesh, in_specs=placed, out_specs=P("sp", "tp"), check_vma=False
    )
```
